32 devices in a mesh: sp: 16 (over z, y, core), tp: 2 (over x).
Axes of the slice: x: 2, y: 2, z: 4, core: 2. Of those that a mesh axis runs over, the one named last changes fastest.
Arguments:
- resid: bfloat16 [4096, 2048], P(('sp', 'tp')), may hold values from -6 to 6
- queries: bfloat16 [4096, 1024], P('sp', 'tp'), may hold values from -6 to 6
- keys: bfloat16 [512, 4096], P('tp', 'sp'), may hold values from -6 to 6
- values: bfloat16 [512, 4096], P('tp', 'sp'), may hold values from -6 to 6
- log_gates: float32 [16, 4096], P('tp', 'sp'), may hold values from -411 to 0, as said below
- q_gain: float32 [64], replicated, may hold values from 0.5 to 7
- k_gain: float32 [64], replicated, may hold values from 0.5 to 7
- w_out: bfloat16 [1024, 2048], P('tp'), may hold values from -0.1875 to 0.1875
- mlp_gain: bfloat16 [2048], replicated, may hold values from 0.099609375 to 1.8984375
- w_up: bfloat16 [2048, 8192], P('sp', 'tp'), may hold values from -0.125 to 0.125
- w_down: bfloat16 [8192, 2048], P('tp', 'sp'), may hold values from -0.0625 to 0.0625
Outputs:
- output: bfloat16 [4096, 2048], P(('sp', 'tp'))
The draws below stay inside these ranges and needn't reach their ends.
Inputs may be any that keep to these rules, and one draw needn't show every extreme that they name: `log_gates`: each head's values never rise along positions.
All inputs are finite; a program needn't handle non-finite values.
Results may differ from the reference program's by a relative error of at most 0.018.
The reference program's roundings to bfloat16 on the way count: a program that leaves them out, or rounds other values in their place, can miss the bound.
Values may be sent and summed in bfloat16 or wider, within the bound.
A program may use at most 128 MiB of HBM per device.

```python
import math
import jax
import jax.numpy as jnp
from jax import lax

D = 2048
QUERY_HEADS = 16
HK = 8
DH = 64
FF = 8192
TOK_DEV = 256
SEQUENCE_TOKENS = 4096
QD = 1024
KD = 512
N_TP = 2


def key_table(key):
    base = jnp.clip(jax.random.normal(jax.random.fold_in(key, 101), (SEQUENCE_TOKENS, KD), jnp.float32), -6.0, 6.0)
    return base


def draw_keys(key, part):
    base = key_table(key)
    return base.T.astype(jnp.bfloat16)


def draw_values(key, part):
    base = jax.random.normal(jax.random.fold_in(key, 121), (KD, SEQUENCE_TOKENS), jnp.float32)
    return jnp.clip(base, -6.0, 6.0).astype(jnp.bfloat16)


def draw_queries(key, part):
    base = jnp.clip(jax.random.normal(jax.random.fold_in(key, 104), (SEQUENCE_TOKENS, QD), jnp.float32), -6.0, 6.0)
    return base.astype(jnp.bfloat16)


def draw_q_gain(key, part):
    return jax.random.uniform(jax.random.fold_in(key, 106), (DH,), jnp.float32, 0.5, 1.5)


def draw_k_gain(key, part):
    return jax.random.uniform(jax.random.fold_in(key, 107), (DH,), jnp.float32, 0.5, 1.5)


def draw_log_gates(key, part):
    share = 0.5
    slow = jax.random.uniform(jax.random.fold_in(key, 111), (QUERY_HEADS,)) < share
    fast_rate = jnp.exp(jax.random.uniform(jax.random.fold_in(key, 112), (QUERY_HEADS, 1), jnp.float32, math.log(1.0 / 50.0), math.log(1.0 / 30.0)))
    blocks = SEQUENCE_TOKENS // TOK_DEV
    block_factor = jnp.exp(jax.random.uniform(jax.random.fold_in(key, 113), (1, blocks, 1), jnp.float32, math.log(0.5), math.log(2.0)))
    rough = jax.random.uniform(jax.random.fold_in(key, 114), (QUERY_HEADS, blocks, TOK_DEV), jnp.float32, 0.5, 1.5)
    raw = (block_factor * rough).reshape(QUERY_HEADS, SEQUENCE_TOKENS)
    slow_total = jax.random.uniform(jax.random.fold_in(key, 115), (QUERY_HEADS, 1), jnp.float32, 0.4, 0.8)
    slow_step = raw * slow_total / jnp.sum(raw, axis=1, keepdims=True)
    fast_step = raw * fast_rate
    advance_loop = jnp.where(slow[:, None], slow_step, fast_step)
    increments = jax.random.randint(jax.random.fold_in(key, 116), (2,), 1, SEQUENCE_TOKENS)
    loss_values = jax.random.uniform(jax.random.fold_in(key, 117), (QUERY_HEADS, 2), jnp.float32, 0.2, 0.5)
    increment_sum = jnp.zeros((QUERY_HEADS, SEQUENCE_TOKENS), jnp.float32).at[:, increments].add(-jnp.log1p(-loss_values))
    return -jnp.cumsum(advance_loop + increment_sum, axis=1)


def steps_of(rng, dims, pieces, smallest, high):
    def one(position, shards_of):
        steps = jax.random.uniform(jax.random.fold_in(jax.random.fold_in(rng, 6), position), (shards_of,), jnp.float32, smallest / len(pieces), high / len(pieces))
        return jnp.repeat(jnp.exp(steps), dims[position] // shards_of).reshape((-1,) + (1,) * (len(dims) - position - 1))

    factor_of = one(*pieces[0])
    for cut in pieces[1:]:
        factor_of = factor_of * one(*cut)
    return factor_of


def bell_draw(rng, dims, scale, most, cuts=(), held_as=jnp.bfloat16):
    values = scale * jax.random.normal(rng, dims, jnp.float32)
    if cuts:
        values = values * steps_of(rng, dims, cuts, -0.22, 0.18)
    return jnp.clip(values, -most, most).astype(held_as)


def setup_inputs(seed: int = 0) -> dict:
    arg_keys = jax.random.split(jax.random.key(seed), 12)
    resid = bell_draw(arg_keys[0], (SEQUENCE_TOKENS, D), 1.0, 6.0, ((0, 32),))
    queries = draw_queries(jax.random.fold_in(arg_keys[11], 71), 0)
    keys = draw_keys(jax.random.fold_in(arg_keys[11], 71), 0)
    values = draw_values(jax.random.fold_in(arg_keys[11], 71), 0)
    log_gates = draw_log_gates(jax.random.fold_in(arg_keys[11], 71), 0)
    q_gain = draw_q_gain(jax.random.fold_in(arg_keys[11], 71), 0)
    k_gain = draw_k_gain(jax.random.fold_in(arg_keys[11], 71), 0)
    w_out = bell_draw(arg_keys[7], (QD, D), QD ** -0.5, 0.1875, ((0, 2),))
    mlp_gain = jnp.clip(1.0 + 0.18 * jax.random.normal(arg_keys[8], (D,), jnp.float32), 0.099609375, 1.8984375).astype(jnp.bfloat16)
    w_up = bell_draw(arg_keys[9], (D, FF), D ** -0.5, 0.125, ((0, 16), (1, 2)))
    w_down = bell_draw(arg_keys[10], (FF, D), FF ** -0.5, 0.0625, ((0, 2), (1, 16)))
    return {"resid": resid, "queries": queries, "keys": keys, "values": values, "log_gates": log_gates, "q_gain": q_gain, "k_gain": k_gain, "w_out": w_out, "mlp_gain": mlp_gain, "w_up": w_up, "w_down": w_down}


EPS = 1e-06

def rms_last(input_values, gain):
    scale = lax.rsqrt(lax.optimization_barrier(jnp.mean(input_values * input_values, axis=-1, keepdims=True)) + EPS)
    return input_values * scale * gain

def reference(resid, queries, keys, values, log_gates, q_gain, k_gain, w_out, mlp_gain, w_up, w_down):
    group = QUERY_HEADS // HK
    query_heads = queries.astype(jnp.float32).reshape(SEQUENCE_TOKENS, QUERY_HEADS, DH)
    qnorm = (rms_last(query_heads, q_gain) * DH ** (-0.5)).astype(jnp.bfloat16).astype(jnp.float32)
    key_heads = keys.astype(jnp.float32).T.reshape(SEQUENCE_TOKENS, HK, DH)
    knorm = rms_last(key_heads, k_gain).astype(jnp.bfloat16).astype(jnp.float32)
    value_heads = values.astype(jnp.float32).T.reshape(SEQUENCE_TOKENS, HK, DH)
    qblock = math.gcd(SEQUENCE_TOKENS, 256)
    key_gates = log_gates.reshape(HK, group, 1, SEQUENCE_TOKENS)
    key_pos = jnp.arange(SEQUENCE_TOKENS, dtype=jnp.int32)

    def one_block(start):
        qrows = lax.dynamic_slice_in_dim(qnorm, start, qblock, 0).reshape(qblock, HK, group, DH)
        qgates = lax.dynamic_slice_in_dim(log_gates, start, qblock, 1).reshape(HK, group, qblock)
        logits = jnp.einsum('qkgd,skd->kgqs', qrows, knorm) + qgates[..., None] - key_gates
        qpos = start + jnp.arange(qblock, dtype=jnp.int32)
        logits = jnp.where(key_pos[None, :] <= qpos[:, None], logits, -jnp.inf)
        top = lax.optimization_barrier(jnp.max(logits, axis=-1, keepdims=True))
        weights = jnp.exp(logits - top)
        denom = lax.optimization_barrier(jnp.sum(weights, axis=-1))
        probs = lax.optimization_barrier(weights.astype(jnp.bfloat16)).astype(jnp.float32)
        summed = jnp.einsum('kgqs,skd->qkgd', probs, value_heads)
        result = summed / jnp.transpose(denom, (2, 0, 1))[..., None]
        return result.reshape(qblock, QD).astype(jnp.bfloat16)
    starts = (jnp.arange(SEQUENCE_TOKENS // qblock) * qblock).astype(jnp.int32)
    attn = lax.map(one_block, starts).reshape(SEQUENCE_TOKENS, QD)
    proj = jnp.dot(attn, w_out, preferred_element_type=jnp.float32)
    mixed = (resid.astype(jnp.float32) + proj).astype(jnp.bfloat16)
    normed = rms_last(mixed.astype(jnp.float32), mlp_gain.astype(jnp.float32)).astype(jnp.bfloat16)
    upward = jnp.dot(normed, w_up, preferred_element_type=jnp.float32)
    act = jnp.square(jax.nn.relu(upward)).astype(jnp.bfloat16)
    width = FF // N_TP
    summed_down = jnp.zeros((SEQUENCE_TOKENS, D), jnp.float32)
    for index in range(N_TP):
        partial_value = jnp.dot(act[:, index * width:(index + 1) * width], w_down[index * width:(index + 1) * width], preferred_element_type=jnp.float32).astype(jnp.bfloat16)
        summed_down = summed_down + lax.optimization_barrier(partial_value).astype(jnp.float32)
    return (mixed.astype(jnp.float32) + summed_down).astype(jnp.bfloat16)
```

```python
import functools
import math

import jax
import jax.numpy as jnp
from jax import lax
from jax.experimental import pallas as pl
from jax.experimental.pallas import tpu as pltpu
from jax.sharding import PartitionSpec as P


EPS = 1e-06
LANES = 128
BF = jnp.bfloat16
F32 = jnp.float32


def rms_last(input_values, gain):
    scale = lax.rsqrt(jnp.mean(input_values * input_values, axis=-1, keepdims=True) + EPS)
    return input_values * scale * gain


def split3(x):
    hi = lax.reduce_precision(x, 8, 7)
    mid = lax.reduce_precision(x - hi, 8, 7)
    low = lax.reduce_precision(x - hi - mid, 8, 7)
    return hi.astype(BF), mid.astype(BF), low.astype(BF)


def shifted(x, axis, delta):
    size = lax.axis_size(axis)
    return lax.ppermute(x, axis, [(i, (i + delta) % size) for i in range(size)])


def exchanged(x, axis, mask):
    size = lax.axis_size(axis)
    return lax.ppermute(x, axis, [(i, i ^ mask) for i in range(size)])


def ring_parts(x, axis, stride):
    count = lax.axis_size(axis) // stride
    rows = x.shape[0]
    out = [(0, 0, x)]
    forward = backward = x
    for step in range(1, (count - 1) // 2 + 1):
        forward = shifted(forward, axis, stride)
        backward = shifted(backward, axis, -stride)
        out += [(step, 0, forward), (count - step, 0, backward)]
    if count % 2 == 0:
        step = count // 2
        half = rows // 2 if count > 2 else rows
        out.append((step, 0, shifted(forward[:half], axis, stride)))
        if half < rows:
            out.append((step, half, shifted(backward[half:], axis, -stride)))
    return out


def attention_kernel(
    arrays, heads, group, head_size, positions, chunks, ids_ref, me_ref, q_ref, gate_ref, *refs
):
    pieces = refs[:arrays]
    out_ref, rhs_ref, top_ref, total_ref, sum_ref = refs[-5:]
    me = me_ref[0]
    top_ref[...] = jnp.full_like(top_ref, -1e30)
    total_ref[...] = jnp.zeros_like(total_ref)
    sum_ref[...] = jnp.zeros_like(sum_ref)
    width = group * positions
    value_rows = heads * head_size
    query_count = heads * group
    row = lax.broadcasted_iota(jnp.int32, (LANES, width), 0)
    column = lax.broadcasted_iota(jnp.int32, (LANES, width), 1) // positions
    for head in range(heads):
        picked = head * group + column
        pick = (row == picked) | (row == query_count + picked) | (row == 2 * query_count + picked)
        tail = jnp.where(pick, 1.0, 0.0)
        for part in range(3):
            gates = jnp.broadcast_to(gate_ref[head, part : part + 1, :], (LANES, width))
            tail = jnp.where(row == 3 * query_count + part, gates, tail)
        rhs_ref[head, :LANES, :] = jnp.zeros((LANES, width), BF)
        slot = head * head_size % LANES
        rhs_ref[head, slot : slot + head_size, :] = q_ref[head]
        rhs_ref[head, LANES:, :] = tail.astype(BF)

    def block(piece, index, masked):
        gates = piece[index, chunks * positions : (chunks + 1) * positions, :]
        base = (chunks + 1) * positions
        for head in range(heads):
            chunk = head * head_size // LANES
            lhs = jnp.concatenate(
                [piece[index, chunk * positions : (chunk + 1) * positions, :], gates], axis=1
            )
            logits = jnp.dot(lhs, rhs_ref[head], preferred_element_type=F32)
            if masked:
                key_pos = lax.broadcasted_iota(jnp.int32, (positions, width), 0)
                query_pos = lax.broadcasted_iota(jnp.int32, (positions, width), 1) % positions
                logits = jnp.where(key_pos <= query_pos, logits, -jnp.inf)
            old_top = top_ref[head]
            new_top = jnp.maximum(old_top, jnp.max(logits, axis=0, keepdims=True))
            rescale = jnp.exp(old_top - new_top)
            weights = jnp.exp(logits - new_top)
            total_ref[head] = total_ref[head] * rescale + jnp.sum(weights, axis=0, keepdims=True)
            top_ref[head] = new_top
            first = base + head * head_size
            value = jnp.concatenate(
                [
                    piece[index, first + c * value_rows : first + c * value_rows + head_size, :]
                    for c in range(positions // LANES)
                ],
                axis=1,
            )
            sum_ref[head] = sum_ref[head] * rescale + jnp.dot(
                value, weights.astype(BF), preferred_element_type=F32
            )

    block(pieces[0], 0, True)
    per = pieces[0].shape[0]
    for number in range(arrays):

        def body(index, carry, number=number):
            @pl.when(ids_ref[number * per + index] < me)
            def _():
                block(pieces[number], index, False)

            return carry

        lax.fori_loop(0, per, body, 0)
    for head in range(heads):
        result = sum_ref[head] / total_ref[head]
        for g in range(group):
            first = (head * group + g) * head_size
            out_ref[first : first + head_size, :] = result[
                :, g * positions : (g + 1) * positions
            ].astype(BF)


def hidden_units(rows, up_whole):
    product = jnp.dot(rows, up_whole, preferred_element_type=F32)
    return jnp.square(jax.nn.relu(product)).astype(BF)


def square_tail(own, up_whole, groups):
    rows, half = own.shape[0], own.shape[0] // 2

    def swap(x, mask):
        return exchanged(x, "sp", mask) if mask else exchanged(x, "tp", 1)

    side, across = swap(own, 0), swap(own, 2)
    corner_first, corner_last = swap(across[:half], 0), swap(side[half:], 2)
    mine = [own, side, across, corner_first, corner_last]
    mine_act = hidden_units(jnp.concatenate(mine, axis=0), up_whole)
    other_rows = jnp.concatenate([swap(part, 1) for part in mine], axis=0)
    other_act = hidden_units(other_rows, up_whole)
    cuts = [(3 * rows, 4 * rows), (rows, 3 * rows), (0, rows)]
    out = []
    for weight in groups:
        other = jnp.dot(other_act, weight, preferred_element_type=F32).astype(BF)
        partial = jnp.dot(mine_act, weight, preferred_element_type=F32)
        corner_in, middle_in, own_in = [swap(other[a:b], 1).astype(F32) for a, b in cuts]
        corner = (partial[3 * rows :] + corner_in).astype(BF)
        middle = partial[rows : 3 * rows] + middle_in
        from_across = swap(corner[:half], 2).astype(F32)
        from_side = swap(corner[half:], 0).astype(F32)
        side_sum = jnp.concatenate([middle[:half] + from_across, middle[half:rows]], axis=0)
        across_sum = jnp.concatenate([middle[rows:-half], middle[-half:] + from_side], axis=0)
        side_out = swap(side_sum.astype(BF), 0).astype(F32)
        across_out = swap(across_sum.astype(BF), 2).astype(F32)
        out.append(partial[:rows] + own_in + side_out + across_out)
    return out


def general_tail(normed, up_whole, down_whole, inner, tp):
    share = normed.shape[0]
    rows_all = jnp.concatenate(
        [normed] + [shifted(normed, "tp", step) for step in range(1, tp)], axis=0
    )
    bit = inner // 2
    while bit:
        rows_all = jnp.concatenate([rows_all, exchanged(rows_all, "sp", bit)], axis=0)
        bit //= 2
    act = hidden_units(rows_all, up_whole)
    partial = jnp.dot(act, down_whole, preferred_element_type=F32)
    bit = 1
    while bit < inner:
        half = partial.shape[0] // 2
        partial = partial[:half] + exchanged(partial[half:].astype(BF), "sp", bit).astype(F32)
        bit *= 2
    total = partial[:share]
    for step in range(1, tp):
        block = partial[step * share : (step + 1) * share].astype(BF)
        total = total + shifted(block, "tp", -step).astype(F32)
    return total


def local(resid, queries, keys, values, log_gates, q_gain, k_gain, w_out, mlp_gain, w_up, w_down):
    sp, tp = lax.axis_size("sp"), lax.axis_size("tp")
    me, my_tp = lax.axis_index("sp"), lax.axis_index("tp")
    inner = math.gcd(sp, 4)
    outer = sp // inner
    my_inner, my_outer = me % inner, me // inner
    positions = queries.shape[0]
    head_size = q_gain.shape[0]
    query_count = log_gates.shape[0]
    heads = keys.shape[0] // head_size
    group = query_count // heads

    key_heads = keys.astype(F32).reshape(heads, head_size, positions)
    key_scale = lax.rsqrt(jnp.mean(key_heads * key_heads, axis=1, keepdims=True) + EPS)
    knorm = (key_heads * key_scale * k_gain[None, :, None]).astype(BF)
    knorm = knorm.reshape(heads * head_size, positions).T
    chunks = -(-heads * head_size // LANES)
    knorm = jnp.pad(knorm, ((0, 0), (0, chunks * LANES - heads * head_size)))
    gate_parts = split3(log_gates)
    gate_block = jnp.concatenate(
        [-part.T for part in gate_parts]
        + [jnp.ones((positions, 3), BF), jnp.zeros((positions, LANES - 3 * query_count - 3), BF)],
        axis=1,
    )
    packed = jnp.concatenate(
        [knorm[:, c * LANES : (c + 1) * LANES] for c in range(chunks)]
        + [gate_block]
        + [values[:, c * LANES : (c + 1) * LANES] for c in range(positions // LANES)],
        axis=0,
    )
    rows = packed.shape[0]
    ring = sorted(ring_parts(packed, "sp", inner), key=lambda part: part[:2])
    stacked = jnp.concatenate([part[2] for part in ring], axis=0).reshape(outer, rows, LANES)
    arrays, masks = [stacked], [0]
    bit = inner // 2
    while bit:
        arrays += [exchanged(a, "sp", bit) for a in arrays]
        masks += [mask ^ bit for mask in masks]
        bit //= 2
    back = jnp.arange(outer, dtype=jnp.int32)
    ids = jnp.concatenate(
        [((my_outer - back) % outer) * inner + (my_inner ^ mask) for mask in masks]
    ).astype(jnp.int32)

    hidden = w_up.shape[1] // inner
    depth = w_up.shape[0]

    def spread(piece_for, axis):
        own = piece_for(my_inner)
        size = own.shape[axis]
        shape = list(own.shape)
        shape[axis] *= inner
        whole = jnp.zeros(shape, BF)
        whole = lax.dynamic_update_slice_in_dim(whole, own, my_inner * size, axis)
        for mask in range(1, inner):
            got = exchanged(piece_for(my_inner ^ mask), "sp", mask)
            whole = lax.dynamic_update_slice_in_dim(whole, got, (my_inner ^ mask) * size, axis)
        return whole

    up_part = spread(lambda e: lax.dynamic_slice_in_dim(w_up, e * hidden, hidden, 1), 0)
    down_part = spread(lambda e: lax.dynamic_slice_in_dim(w_down, e * hidden, hidden, 0), 1)
    up_ring = ring_parts(up_part, "sp", inner)
    down_ring = ring_parts(down_part, "sp", inner)
    early = [part for _, _, part in up_ring[1:3]]

    query_heads = queries.astype(F32).reshape(positions, query_count, head_size)
    qnorm = (rms_last(query_heads, q_gain) * head_size ** (-0.5)).astype(BF)
    qt = jnp.transpose(qnorm.reshape(positions, heads, group, head_size), (1, 3, 2, 0))
    qt = qt.reshape(heads, head_size, group * positions)
    own_gates = jnp.stack([part.astype(F32) for part in gate_parts], axis=1)
    own_gates = own_gates.reshape(heads, group, 3, positions).transpose(0, 2, 1, 3)
    own_gates = own_gates.reshape(heads, 3, group * positions)

    smem = pl.BlockSpec(memory_space=pltpu.SMEM)
    vmem = pl.BlockSpec(memory_space=pltpu.VMEM)
    width = group * positions
    attn = pl.pallas_call(
        functools.partial(
            attention_kernel, len(arrays), heads, group, head_size, positions, chunks
        ),
        out_shape=jax.ShapeDtypeStruct((query_count * head_size, positions), BF),
        in_specs=[smem, smem, vmem, vmem] + [vmem] * len(arrays)
        + [pl.BlockSpec(memory_space=pl.ANY)] * len(early),
        out_specs=vmem,
        scratch_shapes=[
            pltpu.VMEM((heads, 2 * LANES, width), BF),
            pltpu.VMEM((heads, 1, width), F32),
            pltpu.VMEM((heads, 1, width), F32),
            pltpu.VMEM((heads, head_size, width), F32),
        ],
        compiler_params=pltpu.CompilerParams(vmem_limit_bytes=40 * 1024 * 1024),
        cost_estimate=pl.CostEstimate(
            flops=6 * sp * heads * width * positions * LANES,
            bytes_accessed=2 * sp * rows * LANES,
            transcendentals=sp * heads * width * positions,
        ),
    )(ids, me.astype(jnp.int32).reshape(1), qt, own_gates, *arrays, *early)

    up_whole = jnp.zeros((depth * sp, hidden), BF)
    for step, first, part in up_ring:
        start = ((my_outer - step) % outer) * up_part.shape[0] + first
        up_whole = lax.dynamic_update_slice(up_whole, part, (start, 0))
    share = positions // tp
    proj = jnp.zeros((share, resid.shape[1]), F32)
    weight = w_out
    for step in range(tp):
        target = (my_tp + step) % tp
        mine = lax.dynamic_slice_in_dim(attn, target * share, share, 1)
        if step:
            mine = shifted(mine, "tp", step)
            weight = shifted(weight, "tp", 1)
        proj = proj + lax.dot_general(
            mine, weight, (((0,), (0,)), ((), ())), preferred_element_type=F32
        )
    mixed = (resid.astype(F32) + proj).astype(BF)
    normed = rms_last(mixed.astype(F32), mlp_gain.astype(F32)).astype(BF)

    if tp == 2 and inner == 4:
        by_step = {}
        for step, first, part in down_ring:
            by_step.setdefault(step, []).append(part)
        last = outer // 2
        steps = [step for step in by_step if step != last]
        whole = {step: jnp.concatenate(parts, axis=0) for step, parts in by_step.items()}
        groups = [jnp.concatenate([whole[step] for step in steps], axis=1), whole[last]]
        wide = whole[last].shape[1]
        totals = square_tail(normed, up_whole, groups)
        total = jnp.zeros(mixed.shape, F32)
        for number, step in enumerate(steps + [last]):
            start = ((my_outer - step) % outer) * wide
            piece = totals[1] if step == last else totals[0][:, number * wide : (number + 1) * wide]
            total = lax.dynamic_update_slice_in_dim(total, piece, start, 1)
    else:
        down_whole = jnp.zeros((hidden, depth * sp), BF)
        for step, first, part in down_ring:
            start = ((my_outer - step) % outer) * down_part.shape[1]
            down_whole = lax.dynamic_update_slice(down_whole, part, (first, start))
        total = general_tail(normed, up_whole, down_whole, inner, tp)
    return (mixed.astype(F32) + total).astype(BF)


def solution(mesh):
    return jax.shard_map(
        local,
        mesh=mesh,
        in_specs=(
            P(("sp", "tp"), None),
            P("sp", "tp"),
            P("tp", "sp"),
            P("tp", "sp"),
            P("tp", "sp"),
            P(),
            P(),
            P("tp", None),
            P(),
            P("sp", "tp"),
            P("tp", "sp"),
        ),
        out_specs=P(("sp", "tp"), None),
        check_vma=False,
    )
```
